512 devices in a mesh: dp: 4 (over x), kv: 64 (over z, y), tp: 2 (over core).
Axes of the slice: x: 4, y: 8, z: 8, core: 2. Of those that a mesh axis runs over, the one named last changes fastest.
Arguments:
- token_state: bfloat16 [64, 4096], P('dp', 'kv'), may hold values from -150 to 150
- norm_gain: float32 [4096], P('kv'), may hold values from 0.1 to 1.9
- wq_nope: bfloat16 [4096, 1024], P('kv', 'tp'), may hold values from -0.09375 to 0.09375
- wq_rope: bfloat16 [4096, 512], P('kv', 'tp'), may hold values from -0.09375 to 0.09375
- w_latent: bfloat16 [4096, 512], P('kv'), may hold values from -0.09375 to 0.09375
- w_rope_key: bfloat16 [4096, 32], P('kv'), may hold values from -0.09375 to 0.09375
- kv_gain: float32 [512], replicated, may hold values from 0.1 to 1.9
- w_uk: bfloat16 [512, 1024], P('kv', 'tp'), may hold values from -0.25 to 0.25
- w_uv: bfloat16 [512, 1024], P('kv', 'tp'), may hold values from -6 to 6
- w_out: bfloat16 [1024, 4096], P('tp', 'kv'), may hold values from -0.1875 to 0.1875
- latent_cache: bfloat16 [64, 12288, 512], P('dp', 'kv'), may hold values from -500 to 500
- rope_cache: bfloat16 [64, 32, 12288], P('dp', None, 'kv'), may hold values from -6 to 6
- lengths: int32 [64], P('dp'), may hold values from 3072 to 12287, as said below
Outputs:
- mixed: bfloat16 [64, 4096], P('dp', ('kv', 'tp'))
- latent_new: bfloat16 [64, 512], P('dp')
- rope_new: bfloat16 [64, 32], P('dp')
The draws below stay inside these ranges and needn't reach their ends.
Inputs may be any that keep to these rules, and one draw needn't show every extreme that they name: Sequence b has cached positions 0 to lengths[b] - 1 and its new token takes position lengths[b]; in each aligned block of 16 sequences one has length 12287.
All inputs are finite; a program needn't handle non-finite values.
Results may differ from the reference program's by a relative error of at most 0.02.
Values may be sent and summed in bfloat16 or wider, within the bound.
No kernel may reach another device: no remote copies, remote signals or barrier semaphores. Data moves between devices by JAX's collectives and lax.ppermute only.
A program may use at most 64 MiB of HBM per device.

```python
import jax
import jax.numpy as jnp
from jax import lax

D = 4096
HEADS = 16
NOPE = 64
ROPE = 32
V_DIM = 64
RANK = 512
SEQS_DEV = 16
BATCH = 64
POSITIONS = 12288
N_TP = 2


def draw_token_state(key, part):
    columns = jnp.arange(D, dtype=jnp.float32) / D
    col_scale = jnp.exp(jnp.log(5.0) * columns)
    sample = jnp.clip(jax.random.normal(key, (BATCH, D), jnp.float32), -6.0, 6.0)
    return (sample * col_scale[None, :]).astype(jnp.bfloat16)


def draw_latent_cache(key, part):
    shape = (BATCH, POSITIONS, RANK)
    sample = jnp.clip(jax.random.normal(key, shape, jnp.float32), -6.0, 6.0)
    return sample.astype(jnp.bfloat16)


def draw_lengths(key, part):
    groups = BATCH // SEQS_DEV
    sample = jax.random.randint(key, (groups, SEQS_DEV), POSITIONS // 4, POSITIONS)
    chosen = jax.random.randint(jax.random.fold_in(key, 1), (groups, 1), 0, SEQS_DEV)
    slots = jnp.arange(SEQS_DEV, dtype=jnp.int32)[None, :]
    sample = jnp.where(slots == chosen, POSITIONS - 1, sample)
    return sample.reshape(BATCH).astype(jnp.int32)


def level_of(rng, shape, cuts, low, high):
    level = 1.0
    for axis_at, shards_of in cuts:
        steps = jax.random.uniform(jax.random.fold_in(jax.random.fold_in(rng, 6), axis_at), (shards_of,), jnp.float32, low / len(cuts), high / len(cuts))
        level = level * jnp.repeat(jnp.exp(steps), shape[axis_at] // shards_of).reshape((-1,) + (1,) * (len(shape) - 1 - axis_at))
    return level


def centred(stream_key, dims, width, most, cuts=(), held_as=jnp.bfloat16):
    gain = level_of(stream_key, dims, cuts, -0.22, 0.18) if cuts else 1.0
    array = jax.random.normal(stream_key, dims, jnp.float32) * width * gain
    return jnp.minimum(jnp.maximum(array, -most), most).astype(held_as)


def setup_inputs(seed: int = 0) -> dict:
    key_list = jax.random.split(jax.random.key(seed), 14)
    return {
        "token_state": draw_token_state(jax.random.fold_in(key_list[13], 71), 0),
        "norm_gain": jnp.clip(1.0 + 0.18 * jax.random.normal(key_list[1], (D,), jnp.float32), 0.1, 1.9),
        "wq_nope": centred(key_list[2], (D, HEADS * NOPE), D ** -0.5, 0.09375, ((0, 64), (1, 2))),
        "wq_rope": centred(key_list[3], (D, HEADS * ROPE), D ** -0.5, 0.09375, ((0, 64), (1, 2))),
        "w_latent": centred(key_list[4], (D, RANK), D ** -0.5, 0.09375, ((0, 64),)),
        "w_rope_key": centred(key_list[5], (D, ROPE), D ** -0.5, 0.09375, ((0, 64),)),
        "kv_gain": jnp.clip(1.0 + 0.18 * jax.random.normal(key_list[6], (RANK,), jnp.float32), 0.1, 1.9),
        "w_uk": centred(key_list[7], (RANK, HEADS * NOPE), RANK ** -0.5, 0.25, ((0, 64), (1, 2))),
        "w_uv": centred(key_list[8], (RANK, HEADS * V_DIM), (0.25 * (POSITIONS // 256 + 1) ** 0.5), 6.0, ((0, 64), (1, 2))),
        "w_out": centred(key_list[9], (HEADS * V_DIM, D), (HEADS * V_DIM) ** -0.5, 0.1875, ((0, 2), (1, 64))),
        "latent_cache": draw_latent_cache(jax.random.fold_in(key_list[13], 71), 0),
        "rope_cache": centred(key_list[11], (BATCH, ROPE, POSITIONS), 1.0, 6.0, ((0, 4), (2, 64))),
        "lengths": draw_lengths(jax.random.fold_in(key_list[13], 71), 0),
    }


EPS = 1e-06
THETA = 10000.0
NEG = -1e+30

def rotate(vector, angles):
    half_dim = vector.shape[-1] // 2
    cosine = jnp.cos(angles)
    sine_part = jnp.sin(angles)
    leading = vector[..., :half_dim]
    trailing = vector[..., half_dim:]
    return jnp.concatenate([leading * cosine - trailing * sine_part, trailing * cosine + leading * sine_part], axis=-1)

def rope_angles(lengths):
    half_dim = ROPE // 2
    inv_freq = THETA ** (-jnp.arange(half_dim, dtype=jnp.float32) * 2.0 / ROPE)
    return lengths.astype(jnp.float32)[:, None] * inv_freq[None, :]

def reference(token_state, norm_gain, wq_nope, wq_rope, w_latent, w_rope_key, kv_gain, w_uk, w_uv, w_out, latent_cache, rope_cache, lengths):
    x_wide = token_state.astype(jnp.float32)
    inv_rms = lax.rsqrt(lax.optimization_barrier(jnp.sum(x_wide * x_wide, axis=1, keepdims=True)) / D + EPS)
    scaled = (x_wide * norm_gain).astype(jnp.bfloat16)
    q_nope = jnp.dot(scaled, wq_nope, preferred_element_type=jnp.float32) * inv_rms
    q_rope = jnp.dot(scaled, wq_rope, preferred_element_type=jnp.float32) * inv_rms
    latent_raw = jnp.dot(scaled, w_latent, preferred_element_type=jnp.float32) * inv_rms
    key_raw = jnp.dot(scaled, w_rope_key, preferred_element_type=jnp.float32) * inv_rms
    latent_new = (latent_raw * lax.rsqrt(lax.optimization_barrier(jnp.mean(latent_raw * latent_raw, axis=1, keepdims=True)) + EPS) * kv_gain).astype(jnp.bfloat16)
    angles = rope_angles(lengths)
    rope_new = rotate(key_raw, angles).astype(jnp.bfloat16)
    q_rot = rotate(q_rope.reshape(BATCH, HEADS, ROPE), angles[:, None, :]).astype(jnp.bfloat16)
    q_low = q_nope.astype(jnp.bfloat16).reshape(BATCH, HEADS, NOPE)
    q_latent = jnp.einsum('bhn,rhn->bhr', lax.optimization_barrier(q_low).astype(jnp.float32), w_uk.reshape(RANK, HEADS, NOPE).astype(jnp.float32)).astype(jnp.bfloat16)
    score_scale = (NOPE + ROPE) ** (-0.5)
    positions = jnp.arange(POSITIONS, dtype=jnp.int32)

    def per_sequence(items):
        query_lat, query_rot, latents, rope_rows, new_lat, new_rope, limit = items
        cached = jnp.dot(query_lat, latents.T, preferred_element_type=jnp.float32) + jnp.dot(query_rot, rope_rows, preferred_element_type=jnp.float32)
        own = jnp.dot(query_lat, new_lat[:, None], preferred_element_type=jnp.float32)[:, 0] + jnp.dot(query_rot, new_rope[:, None], preferred_element_type=jnp.float32)[:, 0]
        is_valid = positions < limit
        masked = jnp.where(is_valid[None, :], cached * score_scale, NEG)
        own = own * score_scale
        highest = jnp.maximum(lax.optimization_barrier(jnp.max(masked, axis=1)), own)
        weights = jnp.where(is_valid[None, :], jnp.exp(masked - highest[:, None]), 0.0)
        own_weight = jnp.exp(own - highest)
        totals = lax.optimization_barrier(jnp.sum(weights, axis=1)) + own_weight
        own_low = lax.optimization_barrier(own_weight.astype(jnp.bfloat16)).astype(jnp.float32)
        weighted = jnp.dot(weights.astype(jnp.bfloat16), latents, preferred_element_type=jnp.float32) + own_low[:, None] * new_lat.astype(jnp.float32)[None, :]
        return (weighted, totals)
    weighted, totals = lax.map(per_sequence, (q_latent, q_rot, latent_cache, rope_cache, latent_new, rope_new, lengths))
    weighted_low = lax.optimization_barrier(weighted.astype(jnp.bfloat16)).astype(jnp.float32)
    values = jnp.einsum('bhr,rhv->bhv', weighted_low, w_uv.reshape(RANK, HEADS, V_DIM).astype(jnp.float32)) / totals[:, :, None]
    attended = values.astype(jnp.bfloat16).reshape(BATCH, HEADS * V_DIM)
    group = HEADS * V_DIM // N_TP
    mixed = jnp.zeros((BATCH, D), jnp.float32)
    for index in range(N_TP):
        partial_out = jnp.dot(attended[:, index * group:(index + 1) * group], w_out[index * group:(index + 1) * group], preferred_element_type=jnp.float32)
        mixed = mixed + lax.optimization_barrier(partial_out.astype(jnp.bfloat16)).astype(jnp.float32)
    return (mixed.astype(jnp.bfloat16), latent_new, rope_new)
```

```python
import jax
import jax.numpy as jnp
from jax import lax
from jax.experimental import pallas as pl
from jax.experimental.pallas import tpu as pltpu
from jax.sharding import PartitionSpec as P

D = 4096
NOPE = 64
ROPE = 32
V_DIM = 64
RANK = 512
EPS = 1e-06
THETA = 10000.0
NEG = -1e30
SCALE = (NOPE + ROPE) ** (-0.5)
F32 = jnp.float32
BF16 = jnp.bfloat16
INTERPRET = False


def call(kernel, outs, *args, smem=(), scratch=()):
    specs = [
        pl.BlockSpec(memory_space=pltpu.SMEM if i in smem else pltpu.VMEM) for i in range(len(args))
    ]
    return pl.pallas_call(
        kernel,
        out_shape=tuple(jax.ShapeDtypeStruct(s, d) for s, d in outs),
        in_specs=specs,
        out_specs=tuple(pl.BlockSpec(memory_space=pltpu.VMEM) for _ in outs),
        scratch_shapes=list(scratch),
        interpret=INTERPRET,
    )(*args)


def split2(v):
    high = v.astype(BF16).astype(F32)
    return high, v - high


def split3(v):
    high, rest = split2(v)
    mid, low = split2(rest)
    return high, mid, low


def lanes(shape):
    return lax.broadcasted_iota(jnp.int32, shape, len(shape) - 1)


def project(x_ref, gain_ref, wn_ref, wr_ref, wl_ref, wk_ref, uk_ref, uv_ref, out_ref, buf):
    x = x_ref[...].astype(F32)
    scaled = (x * gain_ref[...]).astype(BF16)
    nope = jnp.dot(scaled, wn_ref[...], preferred_element_type=F32)
    rope = jnp.dot(scaled, wr_ref[...], preferred_element_type=F32)
    latent = jnp.dot(scaled, wl_ref[...], preferred_element_type=F32)
    key = jnp.dot(scaled, wk_ref[...], preferred_element_type=F32)
    squares = jnp.sum(x * x, axis=1, keepdims=True)
    first = lanes((8, 128)) < 64
    square_row = jnp.where(first, squares[:8], squares[8:])
    uk = uk_ref[...].astype(F32)
    uv = uv_ref[...].astype(F32)
    for h in range(8):
        at = pl.ds(8 * h, 8)
        n = slice(64 * h, 64 * h + 64)
        r = slice(32 * h, 32 * h + 32)
        c = slice(128 * (h // 2), 128 * (h // 2) + 128)
        s = slice(8 * (h % 2), 8 * (h % 2) + 8)
        weights = jnp.concatenate([uk[:, n], uv[:, n]], axis=1)
        buf[at, 0:8, :] = jnp.broadcast_to(weights[None], (8, 8, 128))
        rows = (
            jnp.concatenate([nope[:8, n], nope[8:, n]], axis=1),
            jnp.concatenate([rope[:8, r], key[:8], rope[8:, r], key[8:]], axis=1),
            latent[s, c],
            square_row,
        )
        for i, row in enumerate(rows):
            high, low = split2(row)
            buf[at, 8 + 2 * i, :] = high
            buf[at, 9 + 2 * i, :] = low
    out_ref[...] = buf[...].astype(BF16)


def queries(me_ref, got_ref, turn_ref, out_ref, w_ref, own_ref):
    got = got_ref[...].astype(F32)
    weights = got[:, 0:8, :].reshape(512, 128).astype(BF16)
    w_ref[...] = weights
    total = jnp.sum(got[:, 8:16, :], axis=0)
    nope = total[0:1] + total[1:2]
    rope = total[2:3] + total[3:4]
    latent = total[4:5] + total[5:6]
    inv_rms = lax.rsqrt((total[6:7] + total[7:8]) / D + EPS)
    lane = lanes((1, 128))
    q_low = (nope * inv_rms).astype(BF16).astype(F32)
    turned = pltpu.roll(q_low, 64, 1)
    row = lax.broadcasted_iota(jnp.int32, (8, 128), 0)
    wide = lanes((8, 128))
    q_wide = jnp.where(row < 4, jnp.broadcast_to(q_low, (8, 128)), jnp.broadcast_to(turned, (8, 128)))
    q_wide = jnp.where(wide < 64, q_wide, 0.0)
    q_latent = jnp.zeros((8, 128), F32)
    for c in range(4):
        left = jnp.where(row % 4 == c, q_wide, 0.0).astype(BF16)
        q_latent = q_latent + lax.dot_general(
            left,
            weights[128 * c : 128 * c + 128],
            (((1,), (1,)), ((), ())),
            preferred_element_type=F32,
        )
    turn = rope * inv_rms
    swapped = jnp.where(lane % 32 < 16, pltpu.roll(turn, 112, 1), pltpu.roll(turn, 16, 1))
    rotated = turn * turn_ref[0:1, :] + swapped * turn_ref[1:2, :]
    other = pltpu.roll(inv_rms, 64, 1)
    odd = (me_ref[0] // 8) % 2 == 1
    latent_rms = jnp.where((lane < 64) == odd, other, inv_rms)
    high, low = split2(latent * latent_rms)
    rest = jnp.concatenate([rotated, high, low, jnp.zeros((5, 128), F32)], axis=0)
    block = jnp.concatenate([q_latent, rest], axis=0).astype(BF16)
    own_ref[...] = block.astype(F32)
    out_ref[...] = jnp.broadcast_to(block[None], (64, 16, 128))


def attend(len_ref, me_ref, got_ref, cache_ref, rope_ref, out_ref, q_buf, r_buf, buf):
    for h in range(8):
        for j in range(8):
            piece = got_ref[8 * h + j].astype(F32)
            q_buf[j, :, h, :] = piece[0:8]
            r_buf[j, h : h + 1, :] = piece[8:9]
    base = me_ref[0] * 192
    position = lanes((8, 192)) + base
    first = lanes((8, 128)) < 64
    for j in range(8):
        for s in range(2):
            b = 8 * s + j
            q = jnp.concatenate([q_buf[j, 4 * s + c] for c in range(4)], axis=1).astype(BF16)
            q_rot = r_buf[j][:, 64 * s : 64 * s + 32].astype(BF16)
            keys = cache_ref[b]
            scores = lax.dot_general(
                q, keys, (((1,), (1,)), ((), ())), preferred_element_type=F32
            ) + jnp.dot(q_rot, rope_ref[b], preferred_element_type=F32)
            usable = position < len_ref[b]
            masked = jnp.where(usable, scores * SCALE, NEG)
            top = jnp.max(masked, axis=1, keepdims=True)
            weights = jnp.where(usable, jnp.exp(masked - top), 0.0)
            total = jnp.sum(weights, axis=1, keepdims=True)
            weighted = jnp.dot(weights.astype(BF16), keys, preferred_element_type=F32)
            for c in range(4):
                buf[:, j, 4 * s + c, :] = weighted[:, 128 * c : 128 * c + 128]
            for i, part in enumerate(split3(top)):
                buf[:, j, 8 + 4 * s + i, :] = jnp.broadcast_to(part, (8, 128))
            high, low = split2(total)
            buf[:, j, 11 + 4 * s, :] = jnp.where(first, high, low)
    out_ref[...] = buf[...].reshape(64, 16, 128).astype(BF16)


def new_entries(me_ref, got_ref, gain_ref, latent_ref, rope_ref, own_ref, buf):
    for src in range(64):
        piece = got_ref[src].astype(F32)
        c = src // 16
        b = src % 16
        buf[b : b + 1, 128 * c : 128 * c + 128] = piece[9:10] + piece[10:11]
        if src < 8:
            rope_ref[src : src + 1, :] = piece[8:9, 32:64]
            rope_ref[src + 8 : src + 9, :] = piece[8:9, 96:128]
    raw = buf[...]
    scale = lax.rsqrt(jnp.sum(raw * raw, axis=1, keepdims=True) / RANK + EPS)
    new = (raw * scale * gain_ref[...]).astype(BF16)
    latent_ref[...] = new
    buf[...] = new.astype(F32)
    j = me_ref[0] % 8
    for s in range(2):
        line = buf[pl.ds(j + 8 * s, 1), :]
        for c in range(4):
            own_ref[4 * s + c : 4 * s + c + 1, :] = line[:, 128 * c : 128 * c + 128]


def combine(got_ref, w_ref, own_q_ref, own_lat_ref, out_ref):
    got = got_ref[...].astype(F32)
    latent = own_lat_ref[...]
    query = own_q_ref[0:8, :]
    turned = own_q_ref[8:9, :]
    lane = lanes((1, 128))
    pair = turned * pltpu.roll(turned, 96, 1)
    dots = jnp.sum(query * latent, axis=1, keepdims=True)
    row = lax.broadcasted_iota(jnp.int32, (8, 128), 0)
    sums = []
    totals = []
    for s in range(2):
        here = (lane >= 64 * s) & (lane < 64 * s + 32)
        own = jnp.sum(dots[4 * s : 4 * s + 4], axis=0, keepdims=True) + jnp.sum(
            jnp.where(here, pair, 0.0), axis=1, keepdims=True
        )
        own = own * SCALE
        m = got[:, 8 + 4 * s, :] + got[:, 9 + 4 * s, :] + got[:, 10 + 4 * s, :]
        top = jnp.maximum(jnp.max(m, axis=0, keepdims=True), own)
        factor = jnp.exp(m - top)
        own_weight = jnp.exp(own - top)
        total = jnp.sum(factor * got[:, 11 + 4 * s, :], axis=0, keepdims=True)
        totals.append(total + pltpu.roll(total, 64, 1) + own_weight)
        own_low = own_weight.astype(BF16).astype(F32)
        sums.append(
            jnp.sum(got[:, 4 * s : 4 * s + 4, :] * factor[:, None, :], axis=0)
            + own_low * latent[4 * s : 4 * s + 4]
        )
    weighted_low = jnp.concatenate(sums, axis=0).astype(BF16)
    values = jnp.zeros((8, 128), F32)
    for c in range(4):
        part = jnp.dot(
            weighted_low, w_ref[128 * c : 128 * c + 128, :], preferred_element_type=F32
        )
        values = values + jnp.where(row % 4 == c, part, 0.0)
    front = jnp.sum(values[0:4], axis=0, keepdims=True) / totals[0]
    back = jnp.sum(values[4:8], axis=0, keepdims=True) / totals[1]
    attended = jnp.where(lane < 64, pltpu.roll(front, 64, 1), back).astype(BF16).astype(F32)
    out_ref[...] = jnp.broadcast_to(attended, (64, 128))


def output(tp_ref, got_ref, w_ref, keep_ref, send_ref):
    first = lanes((8, 128)) < 64
    total = jnp.zeros((16, 64), F32)
    for h in range(8):
        a = got_ref[8 * h : 8 * h + 8, :]
        left = jnp.concatenate([jnp.where(first, a, 0.0), jnp.where(first, 0.0, a)], axis=0)
        w = w_ref[64 * h : 64 * h + 64, :]
        total = total + jnp.dot(
            left.astype(BF16), jnp.concatenate([w, w], axis=0), preferred_element_type=F32
        )
    total = total.astype(BF16).astype(F32)
    low = total[:, :32]
    high = total[:, 32:]
    zero = tp_ref[0] == 0
    keep_ref[...] = jnp.where(zero, low, high)
    send_ref[...] = jnp.where(zero, high, low).astype(BF16)


def exchanged(value):
    return lax.all_to_all(value, "kv", split_axis=0, concat_axis=0, tiled=True)


def turn_rows(lengths, me):
    j = me % 8
    pair = jnp.stack([lengths[j], lengths[j + 8]]).astype(F32)
    inv_freq = THETA ** (-jnp.arange(ROPE // 2, dtype=F32) * 2.0 / ROPE)
    angles = pair[:, None] * inv_freq[None, :]
    cosine = jnp.cos(angles)
    sine = jnp.sin(angles)
    cosine = jnp.concatenate([cosine] * 4, axis=1).reshape(1, 128)
    sine = jnp.concatenate([-sine, sine, -sine, sine], axis=1).reshape(1, 128)
    return jnp.concatenate([cosine, sine], axis=0)


def local(
    token_state,
    norm_gain,
    wq_nope,
    wq_rope,
    w_latent,
    w_rope_key,
    kv_gain,
    w_uk,
    w_uv,
    w_out,
    latent_cache,
    rope_cache,
    lengths,
):
    me = lax.axis_index("kv").astype(jnp.int32)
    me_s = me.reshape(1)
    tp_s = lax.axis_index("tp").astype(jnp.int32).reshape(1)
    block = (64, 16, 128)
    (sent,) = call(
        project,
        [(block, BF16)],
        token_state,
        norm_gain.reshape(1, -1),
        wq_nope,
        wq_rope,
        w_latent,
        w_rope_key,
        w_uk,
        w_uv,
        scratch=[pltpu.VMEM(block, F32)],
    )
    sent, weights, own_q = call(
        queries,
        [(block, BF16), ((512, 128), BF16), ((16, 128), F32)],
        me_s,
        exchanged(sent),
        turn_rows(lengths, me),
        smem=(0,),
    )
    arrived = exchanged(sent)
    (sent,) = call(
        attend,
        [(block, BF16)],
        lengths,
        me_s,
        arrived,
        latent_cache,
        rope_cache,
        smem=(0, 1),
        scratch=[
            pltpu.VMEM((8, 8, 8, 128), F32),
            pltpu.VMEM((8, 8, 128), F32),
            pltpu.VMEM((8, 8, 16, 128), F32),
        ],
    )
    latent_new, rope_new, own_latent = call(
        new_entries,
        [((16, 512), BF16), ((16, 32), F32), ((8, 128), F32)],
        me_s,
        arrived,
        kv_gain.reshape(1, -1),
        smem=(0,),
        scratch=[pltpu.VMEM((16, 512), F32)],
    )
    (sent,) = call(combine, [((64, 128), F32)], exchanged(sent), weights, own_q, own_latent)
    arrived = exchanged(sent.reshape(64, 1, 128)).reshape(64, 128)
    keep, send = call(
        output, [((16, 32), F32), ((16, 32), BF16)], tp_s, arrived, w_out, smem=(0,)
    )
    other = lax.ppermute(send, "tp", [(0, 1), (1, 0)])
    mixed = (keep + other.astype(F32)).astype(BF16)
    return (mixed, latent_new, rope_new.astype(BF16))


def solution(mesh):
    in_specs = (
        P("dp", "kv"),
        P("kv"),
        P("kv", "tp"),
        P("kv", "tp"),
        P("kv", None),
        P("kv", None),
        P(),
        P("kv", "tp"),
        P("kv", "tp"),
        P("tp", "kv"),
        P("dp", "kv", None),
        P("dp", None, "kv"),
        P("dp"),
    )
    out_specs = (P("dp", ("kv", "tp")), P("dp", None), P("dp", None))
    return jax.shard_map(local, mesh=mesh, in_specs=in_specs, out_specs=out_specs, check_vma=False)
```

```python
import jax
import jax.numpy as jnp
from jax import lax
from jax.experimental import pallas as pl
from jax.experimental.pallas import tpu as pltpu
from jax.sharding import PartitionSpec as P

D = 4096
NOPE = 64
ROPE = 32
V_DIM = 64
RANK = 512
EPS = 1e-06
THETA = 10000.0
NEG = -1e30
SCALE = (NOPE + ROPE) ** (-0.5)
F32 = jnp.float32
BF16 = jnp.bfloat16
INTERPRET = False


def call(kernel, outs, *args, smem=(), near=(), far=(), results_far=(), scratch=()):
    spaces = [
        pltpu.SMEM if i in smem else pl.ANY if i in far else pltpu.VMEM for i in range(len(args))
    ]
    body = kernel
    shapes = [
        jax.ShapeDtypeStruct(*out) if i in results_far else pltpu.VMEM(*out)
        for i, out in enumerate(outs)
    ]
    if len(outs) == 1 and not results_far:
        shapes.append(pltpu.VMEM((8, 128), F32))

        def body(*refs):
            refs[len(args) + 1][...] = jnp.zeros((8, 128), F32)
            kernel(*refs[: len(args) + 1], *refs[len(args) + 2 :])

    results = pl.pallas_call(
        body,
        out_shape=tuple(shapes),
        in_specs=[pl.BlockSpec(memory_space=space) for space in spaces],
        out_specs=tuple(pl.BlockSpec(memory_space=pltpu.VMEM) for _ in shapes),
        scratch_shapes=list(scratch),
        interpret=INTERPRET,
    )(
        *(
            pltpu.with_memory_space_constraint(a, pltpu.VMEM) if i in near else a
            for i, a in enumerate(args)
        )
    )
    return results[: len(outs)]


def split2(v):
    high = v.astype(BF16).astype(F32)
    return high, v - high


def split3(v):
    high, rest = split2(v)
    mid, low = split2(rest)
    return high, mid, low


def lanes(shape):
    return lax.broadcasted_iota(jnp.int32, shape, len(shape) - 1)


def project(x_ref, gain_ref, wn_ref, wr_ref, wl_ref, wk_ref, uk_ref, uv_ref, out_ref, buf):
    x = x_ref[...].astype(F32)
    scaled = (x * gain_ref[...]).astype(BF16)
    nope = jnp.dot(scaled, wn_ref[...], preferred_element_type=F32)
    rope = jnp.dot(scaled, wr_ref[...], preferred_element_type=F32)
    latent = jnp.dot(scaled, wl_ref[...], preferred_element_type=F32)
    key = lax.dot_general(
        scaled, wk_ref[...], (((1,), (1,)), ((), ())), preferred_element_type=F32
    )
    squares = jnp.sum(x * x, axis=1, keepdims=True)
    first = lanes((8, 128)) < 64
    square_row = jnp.where(first, squares[:8], squares[8:])
    uk = uk_ref[...].astype(F32)
    uv = uv_ref[...].astype(F32)
    for h in range(8):
        at = pl.ds(8 * h, 8)
        n = slice(64 * h, 64 * h + 64)
        r = slice(32 * h, 32 * h + 32)
        c = slice(128 * (h // 2), 128 * (h // 2) + 128)
        s = slice(8 * (h % 2), 8 * (h % 2) + 8)
        weights = jnp.concatenate([uk[:, n], uv[:, n]], axis=1)
        buf[at, 0:8, :] = jnp.broadcast_to(weights[None], (8, 8, 128))
        rows = (
            jnp.concatenate([nope[:8, n], nope[8:, n]], axis=1),
            jnp.concatenate([rope[:8, r], key[:8], rope[8:, r], key[8:]], axis=1),
            latent[s, c],
            square_row,
        )
        for i, row in enumerate(rows):
            high, low = split2(row)
            buf[at, 8 + 2 * i, :] = high
            buf[at, 9 + 2 * i, :] = low
    out_ref[...] = buf[...].astype(BF16)


def queries(me_ref, got_ref, turn_ref, out_ref, w_ref, own_ref):
    got = got_ref[...].astype(F32)
    weights = got[:, 0:8, :].reshape(512, 128).astype(BF16)
    w_ref[...] = weights
    total = jnp.sum(got[:, 8:16, :], axis=0)
    nope = total[0:1] + total[1:2]
    rope = total[2:3] + total[3:4]
    latent = total[4:5] + total[5:6]
    inv_rms = lax.rsqrt((total[6:7] + total[7:8]) / D + EPS)
    lane = lanes((1, 128))
    q_low = (nope * inv_rms).astype(BF16).astype(F32)
    turned = pltpu.roll(q_low, 64, 1)
    row = lax.broadcasted_iota(jnp.int32, (8, 128), 0)
    wide = lanes((8, 128))
    q_wide = jnp.where(row < 4, jnp.broadcast_to(q_low, (8, 128)), jnp.broadcast_to(turned, (8, 128)))
    q_wide = jnp.where(wide < 64, q_wide, 0.0)
    q_latent = jnp.zeros((8, 128), F32)
    for c in range(4):
        left = jnp.where(row % 4 == c, q_wide, 0.0).astype(BF16)
        q_latent = q_latent + lax.dot_general(
            left,
            weights[128 * c : 128 * c + 128],
            (((1,), (1,)), ((), ())),
            preferred_element_type=F32,
        )
    turn = rope * inv_rms
    swapped = jnp.where(lane % 32 < 16, pltpu.roll(turn, 112, 1), pltpu.roll(turn, 16, 1))
    rotated = turn * turn_ref[0:1, :] + swapped * turn_ref[1:2, :]
    other = pltpu.roll(inv_rms, 64, 1)
    odd = (me_ref[0] // 8) % 2 == 1
    latent_rms = jnp.where((lane < 64) == odd, other, inv_rms)
    high, low = split2(latent * latent_rms)
    rest = jnp.concatenate([rotated, high, low, jnp.zeros((5, 128), F32)], axis=0)
    block = jnp.concatenate([q_latent, rest], axis=0).astype(BF16)
    own_ref[...] = block.astype(F32)
    out_ref[...] = jnp.broadcast_to(block[None], (64, 16, 128))


def attend(
    len_ref, me_ref, got_ref, cache_hbm, rope_hbm, out_ref, q_buf, r_buf, buf, cache_ref, rope_ref, sem
):
    copies = []
    for j in range(8):
        for s in range(2):
            b = 8 * s + j
            copies.append(
                (
                    pltpu.make_async_copy(cache_hbm.at[b], cache_ref.at[b], sem.at[0, b]),
                    pltpu.make_async_copy(rope_hbm.at[b], rope_ref.at[b], sem.at[1, b]),
                )
            )
    for pair in copies:
        for copy in pair:
            copy.start()
    for h in range(8):
        for j in range(8):
            piece = got_ref[8 * h + j].astype(F32)
            q_buf[j, :, h, :] = piece[0:8]
            r_buf[j, h : h + 1, :] = piece[8:9]
    base = me_ref[0] * 192
    position = lanes((8, 192)) + base
    first = lanes((8, 128)) < 64
    for j in range(8):
        for s in range(2):
            b = 8 * s + j
            q = jnp.concatenate([q_buf[j, 4 * s + c] for c in range(4)], axis=1).astype(BF16)
            q_rot = r_buf[j][:, 64 * s : 64 * s + 32].astype(BF16)
            for copy in copies[2 * j + s]:
                copy.wait()
            keys = cache_ref[b]
            scores = lax.dot_general(
                q, keys, (((1,), (1,)), ((), ())), preferred_element_type=F32
            ) + jnp.dot(q_rot, rope_ref[b], preferred_element_type=F32)
            usable = position < len_ref[b]
            masked = jnp.where(usable, scores * SCALE, NEG)
            top = jnp.max(masked, axis=1, keepdims=True)
            weights = jnp.where(usable, jnp.exp(masked - top), 0.0)
            total = jnp.sum(weights, axis=1, keepdims=True)
            weighted = jnp.dot(weights.astype(BF16), keys, preferred_element_type=F32)
            for c in range(4):
                buf[:, j, 4 * s + c, :] = weighted[:, 128 * c : 128 * c + 128]
            for i, part in enumerate(split3(top)):
                buf[:, j, 8 + 4 * s + i, :] = jnp.broadcast_to(part, (8, 128))
            high, low = split2(total)
            buf[:, j, 11 + 4 * s, :] = jnp.where(first, high, low)
    out_ref[...] = buf[...].reshape(64, 16, 128).astype(BF16)


def new_entries(
    me_ref, tp_ref, got_ref, gain_ref, w_ref, latent_ref, rope_ref, own_ref, half_ref, buf, turn_buf
):
    for src in range(64):
        piece = got_ref[src].astype(F32)
        c = src // 16
        b = src % 16
        buf[b : b + 1, 128 * c : 128 * c + 128] = piece[9:10] + piece[10:11]
        if src < 8:
            turn_buf[src : src + 1, :] = piece[8:9]
    turned = turn_buf[...]
    rope_ref[...] = jnp.concatenate([turned[:, 32:64], turned[:, 96:128]], axis=0).astype(BF16)
    raw = buf[...]
    scale = lax.rsqrt(jnp.sum(raw * raw, axis=1, keepdims=True) / RANK + EPS)
    new = (raw * scale * gain_ref[...]).astype(BF16)
    latent_ref[...] = new
    buf[...] = new.astype(F32)
    j = me_ref[0] % 8
    for s in range(2):
        line = buf[pl.ds(j + 8 * s, 1), :]
        for c in range(4):
            own_ref[4 * s + c : 4 * s + c + 1, :] = line[:, 128 * c : 128 * c + 128]
    half_ref[...] = jnp.where(tp_ref[0] == 0, w_ref[32:64, :], w_ref[0:32, :])


def combine(got_ref, w_ref, own_q_ref, own_lat_ref, out_ref):
    got = got_ref[...].astype(F32)
    latent = own_lat_ref[...]
    query = own_q_ref[0:8, :]
    turned = own_q_ref[8:9, :]
    lane = lanes((1, 128))
    pair = turned * pltpu.roll(turned, 96, 1)
    dots = jnp.sum(query * latent, axis=1, keepdims=True)
    row = lax.broadcasted_iota(jnp.int32, (8, 128), 0)
    sums = []
    totals = []
    for s in range(2):
        here = (lane >= 64 * s) & (lane < 64 * s + 32)
        own = jnp.sum(dots[4 * s : 4 * s + 4], axis=0, keepdims=True) + jnp.sum(
            jnp.where(here, pair, 0.0), axis=1, keepdims=True
        )
        own = own * SCALE
        m = got[:, 8 + 4 * s, :] + got[:, 9 + 4 * s, :] + got[:, 10 + 4 * s, :]
        top = jnp.maximum(jnp.max(m, axis=0, keepdims=True), own)
        factor = jnp.exp(m - top)
        own_weight = jnp.exp(own - top)
        total = jnp.sum(factor * got[:, 11 + 4 * s, :], axis=0, keepdims=True)
        totals.append(total + pltpu.roll(total, 64, 1) + own_weight)
        own_low = own_weight.astype(BF16).astype(F32)
        sums.append(
            jnp.sum(got[:, 4 * s : 4 * s + 4, :] * factor[:, None, :], axis=0)
            + own_low * latent[4 * s : 4 * s + 4]
        )
    weighted_low = jnp.concatenate(sums, axis=0).astype(BF16)
    values = jnp.zeros((8, 128), F32)
    for c in range(4):
        part = jnp.dot(
            weighted_low, w_ref[128 * c : 128 * c + 128, :], preferred_element_type=F32
        )
        values = values + jnp.where(row % 4 == c, part, 0.0)
    front = jnp.sum(values[0:4], axis=0, keepdims=True) / totals[0]
    back = jnp.sum(values[4:8], axis=0, keepdims=True) / totals[1]
    attended = jnp.where(lane < 64, pltpu.roll(front, 64, 1), back).astype(BF16).astype(F32)
    out_ref[...] = jnp.broadcast_to(attended, (128, 128))


def output(tp_ref, got_ref, w_ref, other_ref, out_ref):
    first = lanes((8, 128)) < 64
    tp = tp_ref[0]
    mixed = jnp.zeros((16, 32), F32)
    for group in range(2):
        pieces = []
        for pair in range(4):
            even = got_ref[pl.ds(32 * pair + group, 8, stride=2), :]
            odd = got_ref[pl.ds(32 * pair + 16 + group, 8, stride=2), :]
            front = jnp.where(first, even, pltpu.roll(odd, 64, 1))
            back = jnp.where(first, pltpu.roll(even, 64, 1), odd)
            pieces.append(jnp.concatenate([front, back], axis=0))
        attended = jnp.concatenate(pieces, axis=1).astype(BF16)
        mine = jnp.where(tp == 0, w_ref[0:32, :], w_ref[32:64, :])
        w = jnp.where(tp == group, mine, other_ref[...])
        part = lax.dot_general(
            attended, w, (((1,), (1,)), ((), ())), preferred_element_type=F32
        )
        mixed = mixed + part.astype(BF16).astype(F32)
    out_ref[...] = mixed.astype(BF16)


def exchanged(value, axes="kv"):
    return lax.all_to_all(value, axes, split_axis=0, concat_axis=0, tiled=True)


def turn_rows(lengths, me):
    j = me % 8
    pair = jnp.stack([lengths[j], lengths[j + 8]]).astype(F32)
    inv_freq = THETA ** (-jnp.arange(ROPE // 2, dtype=F32) * 2.0 / ROPE)
    angles = pair[:, None] * inv_freq[None, :]
    cosine = jnp.cos(angles)
    sine = jnp.sin(angles)
    cosine = jnp.concatenate([cosine] * 4, axis=1).reshape(1, 128)
    sine = jnp.concatenate([-sine, sine, -sine, sine], axis=1).reshape(1, 128)
    return jnp.concatenate([cosine, sine], axis=0)


def local(
    token_state,
    norm_gain,
    wq_nope,
    wq_rope,
    w_latent,
    w_rope_key,
    kv_gain,
    w_uk,
    w_uv,
    w_out,
    latent_cache,
    rope_cache,
    lengths,
):
    me = lax.axis_index("kv").astype(jnp.int32)
    me_s = me.reshape(1)
    tp_s = lax.axis_index("tp").astype(jnp.int32).reshape(1)
    block = (64, 16, 128)
    (sent,) = call(
        project,
        [(block, BF16)],
        token_state,
        norm_gain.reshape(1, -1),
        wq_nope,
        wq_rope,
        w_latent,
        w_rope_key.T,
        w_uk,
        w_uv,
        scratch=[pltpu.VMEM(block, F32)],
    )
    sent, weights, own_q = call(
        queries,
        [(block, BF16), ((512, 128), BF16), ((16, 128), F32)],
        me_s,
        exchanged(sent),
        turn_rows(lengths, me),
        smem=(0,),
        near=(1, 2),
    )
    arrived = exchanged(sent)
    (sent,) = call(
        attend,
        [(block, BF16)],
        lengths,
        me_s,
        arrived,
        latent_cache,
        rope_cache,
        smem=(0, 1),
        near=(2,),
        far=(3, 4),
        scratch=[
            pltpu.VMEM((8, 8, 8, 128), F32),
            pltpu.VMEM((8, 8, 128), F32),
            pltpu.VMEM((8, 8, 16, 128), F32),
            pltpu.VMEM((16, 192, 512), BF16),
            pltpu.VMEM((16, 32, 192), BF16),
            pltpu.SemaphoreType.DMA((2, 16)),
        ],
    )
    latent_new, rope_new, own_latent, half = call(
        new_entries,
        [((16, 512), BF16), ((16, 32), BF16), ((8, 128), F32), ((32, 512), BF16)],
        me_s,
        tp_s,
        arrived,
        kv_gain.reshape(1, -1),
        w_out.T,
        smem=(0, 1),
        near=(2,),
        results_far=(0, 1),
        scratch=[pltpu.VMEM((16, 512), F32), pltpu.VMEM((8, 128), F32)],
    )
    other = lax.ppermute(half, "tp", [(0, 1), (1, 0)])
    (sent,) = call(
        combine,
        [((128, 128), F32)],
        exchanged(sent),
        weights,
        own_q,
        own_latent,
        near=(0, 1, 2, 3),
    )
    arrived = exchanged(sent.reshape(128, 1, 128), ("kv", "tp")).reshape(128, 128)
    (mixed,) = call(
        output,
        [((16, 32), BF16)],
        tp_s,
        arrived,
        w_out.T,
        other,
        smem=(0,),
        near=(1, 3),
        results_far=(0,),
    )
    return (mixed, latent_new, rope_new)


def solution(mesh):
    in_specs = (
        P("dp", "kv"),
        P("kv"),
        P("kv", "tp"),
        P("kv", "tp"),
        P("kv", None),
        P("kv", None),
        P(),
        P("kv", "tp"),
        P("kv", "tp"),
        P("tp", "kv"),
        P("dp", "kv", None),
        P("dp", None, "kv"),
        P("dp"),
    )
    out_specs = (P("dp", ("kv", "tp")), P("dp", None), P("dp", None))
    return jax.shard_map(local, mesh=mesh, in_specs=in_specs, out_specs=out_specs, check_vma=False)
```

```python
import jax
import jax.numpy as jnp
from jax import lax
from jax.experimental import pallas as pl
from jax.experimental.pallas import tpu as pltpu
from jax.sharding import PartitionSpec as P

D = 4096
NOPE = 64
ROPE = 32
V_DIM = 64
RANK = 512
EPS = 1e-06
THETA = 10000.0
NEG = -1e30
SCALE = (NOPE + ROPE) ** (-0.5)
F32 = jnp.float32
BF16 = jnp.bfloat16
INTERPRET = False


def call(kernel, outs, *args, smem=(), near=(), far=(), results_far=(), scratch=()):
    spaces = [
        pltpu.SMEM if i in smem else pl.ANY if i in far else pltpu.VMEM for i in range(len(args))
    ]
    body = kernel
    shapes = [
        jax.ShapeDtypeStruct(*out) if i in results_far else pltpu.VMEM(*out)
        for i, out in enumerate(outs)
    ]
    if len(outs) == 1 and not results_far:
        shapes.append(pltpu.VMEM((8, 128), F32))

        def body(*refs):
            refs[len(args) + 1][...] = jnp.zeros((8, 128), F32)
            kernel(*refs[: len(args) + 1], *refs[len(args) + 2 :])

    results = pl.pallas_call(
        body,
        out_shape=tuple(shapes),
        in_specs=[pl.BlockSpec(memory_space=space) for space in spaces],
        out_specs=tuple(pl.BlockSpec(memory_space=pltpu.VMEM) for _ in shapes),
        scratch_shapes=list(scratch),
        interpret=INTERPRET,
    )(
        *(
            pltpu.with_memory_space_constraint(a, pltpu.VMEM) if i in near else a
            for i, a in enumerate(args)
        )
    )
    return results[: len(outs)]


def split2(v):
    high = v.astype(BF16).astype(F32)
    return high, v - high


def split3(v):
    high, rest = split2(v)
    mid, low = split2(rest)
    return high, mid, low


def lanes(shape):
    return lax.broadcasted_iota(jnp.int32, shape, len(shape) - 1)


def project(x_ref, gain_ref, wn_ref, wr_ref, wl_ref, wk_ref, uk_ref, uv_ref, out_ref, buf):
    x = x_ref[...].astype(F32)
    scaled = (x * gain_ref[...]).astype(BF16)
    nope = jnp.dot(scaled, wn_ref[...], preferred_element_type=F32)
    rope = jnp.dot(scaled, wr_ref[...], preferred_element_type=F32)
    latent = jnp.dot(scaled, wl_ref[...], preferred_element_type=F32)
    key = lax.dot_general(
        scaled, wk_ref[...], (((1,), (1,)), ((), ())), preferred_element_type=F32
    )
    squares = jnp.sum(x * x, axis=1, keepdims=True)
    first = lanes((8, 128)) < 64
    square_row = jnp.where(first, squares[:8], squares[8:])
    uk = uk_ref[...].astype(F32)
    uv = uv_ref[...].astype(F32)
    for h in range(8):
        at = pl.ds(8 * h, 8)
        n = slice(64 * h, 64 * h + 64)
        r = slice(32 * h, 32 * h + 32)
        c = slice(128 * (h // 2), 128 * (h // 2) + 128)
        s = slice(8 * (h % 2), 8 * (h % 2) + 8)
        weights = jnp.concatenate([uk[:, n], uv[:, n]], axis=1)
        buf[at, 0:8, :] = jnp.broadcast_to(weights[None], (8, 8, 128))
        rows = (
            jnp.concatenate([nope[:8, n], nope[8:, n]], axis=1),
            jnp.concatenate([rope[:8, r], key[:8], rope[8:, r], key[8:]], axis=1),
            latent[s, c],
            square_row,
        )
        for i, row in enumerate(rows):
            high, low = split2(row)
            buf[at, 8 + 2 * i, :] = high
            buf[at, 9 + 2 * i, :] = low
    out_ref[...] = buf[...].astype(BF16)


def queries(me_ref, got_ref, turn_ref, out_ref, w_ref, own_ref):
    got = got_ref[...].astype(F32)
    weights = got[:, 0:8, :].reshape(512, 128).astype(BF16)
    w_ref[...] = weights
    total = jnp.sum(got[:, 8:16, :], axis=0)
    nope = total[0:1] + total[1:2]
    rope = total[2:3] + total[3:4]
    latent = total[4:5] + total[5:6]
    inv_rms = lax.rsqrt((total[6:7] + total[7:8]) / D + EPS)
    lane = lanes((1, 128))
    q_low = (nope * inv_rms).astype(BF16).astype(F32)
    turned = pltpu.roll(q_low, 64, 1)
    row = lax.broadcasted_iota(jnp.int32, (8, 128), 0)
    wide = lanes((8, 128))
    q_wide = jnp.where(row < 4, jnp.broadcast_to(q_low, (8, 128)), jnp.broadcast_to(turned, (8, 128)))
    q_wide = jnp.where(wide < 64, q_wide, 0.0)
    q_latent = jnp.zeros((8, 128), F32)
    for c in range(4):
        left = jnp.where(row % 4 == c, q_wide, 0.0).astype(BF16)
        q_latent = q_latent + lax.dot_general(
            left,
            weights[128 * c : 128 * c + 128],
            (((1,), (1,)), ((), ())),
            preferred_element_type=F32,
        )
    turn = rope * inv_rms
    swapped = jnp.where(lane % 32 < 16, pltpu.roll(turn, 112, 1), pltpu.roll(turn, 16, 1))
    rotated = turn * turn_ref[0:1, :] + swapped * turn_ref[1:2, :]
    other = pltpu.roll(inv_rms, 64, 1)
    odd = (me_ref[0] // 8) % 2 == 1
    latent_rms = jnp.where((lane < 64) == odd, other, inv_rms)
    high, low = split2(latent * latent_rms)
    rest = jnp.concatenate([rotated, high, low, jnp.zeros((5, 128), F32)], axis=0)
    block = jnp.concatenate([q_latent, rest], axis=0).astype(BF16)
    own_ref[...] = block.astype(F32)
    out_ref[...] = jnp.broadcast_to(block[None], (64, 16, 128))


def attend(
    len_ref,
    me_ref,
    got_ref,
    cache_hbm,
    rope_hbm,
    out_ref,
    q_buf,
    r_buf,
    buf,
    score_buf,
    weight_buf,
    cache_ref,
    rope_ref,
    sem,
):
    copies = [pltpu.make_async_copy(rope_hbm, rope_ref, sem.at[4])] + [
        pltpu.make_async_copy(
            cache_hbm.at[4 * g : 4 * g + 4], cache_ref.at[4 * g : 4 * g + 4], sem.at[g]
        )
        for g in range(4)
    ]
    for copy in copies:
        copy.start()
    for h in range(8):
        for j in range(8):
            piece = got_ref[8 * h + j].astype(F32)
            q_buf[j, :, h, :] = piece[0:8]
            r_buf[j, h : h + 1, :] = piece[8:9]
    position = lanes((8, 192)) + me_ref[0] * 192
    first = lanes((128, 128)) < 64
    copies[0].wait()
    for b in range(16):
        s, j = divmod(b, 8)
        if b % 4 == 0:
            copies[1 + b // 4].wait()
        q = jnp.concatenate([q_buf[j, 4 * s + c] for c in range(4)], axis=1).astype(BF16)
        q_rot = r_buf[j][:, 64 * s : 64 * s + 32].astype(BF16)
        scores = lax.dot_general(
            q, cache_ref[b], (((1,), (1,)), ((), ())), preferred_element_type=F32
        ) + jnp.dot(q_rot, rope_ref[b], preferred_element_type=F32)
        score_buf[8 * b : 8 * b + 8, :] = jnp.where(position < len_ref[b], scores * SCALE, NEG)
    masked = score_buf[...]
    top = jnp.max(masked, axis=1, keepdims=True)
    weights = jnp.where(masked > 0.5 * NEG, jnp.exp(masked - top), 0.0)
    weight_buf[...] = weights
    high, low = split2(jnp.sum(weights, axis=1, keepdims=True))
    rows = [jnp.broadcast_to(part, (128, 128)) for part in split3(top)]
    rows.append(jnp.where(first, high, low))
    for b in range(16):
        s, j = divmod(b, 8)
        for i, row in enumerate(rows):
            buf[:, j, 8 + 4 * s + i, :] = row[8 * b : 8 * b + 8]
    for b in range(16):
        s, j = divmod(b, 8)
        weighted = jnp.dot(
            weight_buf[8 * b : 8 * b + 8, :].astype(BF16), cache_ref[b], preferred_element_type=F32
        )
        for c in range(4):
            buf[:, j, 4 * s + c, :] = weighted[:, 128 * c : 128 * c + 128]
    out_ref[...] = buf[...].reshape(64, 16, 128).astype(BF16)


def new_entries(
    me_ref, tp_ref, got_ref, gain_ref, w_ref, latent_ref, rope_ref, own_ref, half_ref, buf, turn_buf
):
    for src in range(64):
        piece = got_ref[src].astype(F32)
        c = src // 16
        b = src % 16
        buf[b : b + 1, 128 * c : 128 * c + 128] = piece[9:10] + piece[10:11]
        if src < 8:
            turn_buf[src : src + 1, :] = piece[8:9]
    turned = turn_buf[...]
    rope_ref[...] = jnp.concatenate([turned[:, 32:64], turned[:, 96:128]], axis=0).astype(BF16)
    raw = buf[...]
    scale = lax.rsqrt(jnp.sum(raw * raw, axis=1, keepdims=True) / RANK + EPS)
    new = (raw * scale * gain_ref[...]).astype(BF16)
    latent_ref[...] = new
    buf[...] = new.astype(F32)
    j = me_ref[0] % 8
    for s in range(2):
        line = buf[pl.ds(j + 8 * s, 1), :]
        for c in range(4):
            own_ref[4 * s + c : 4 * s + c + 1, :] = line[:, 128 * c : 128 * c + 128]
    half_ref[...] = jnp.where(tp_ref[0] == 0, w_ref[32:64, :], w_ref[0:32, :])


def combine(got_ref, w_ref, own_q_ref, own_lat_ref, out_ref):
    got = got_ref[...].astype(F32)
    latent = own_lat_ref[...]
    query = own_q_ref[0:8, :]
    turned = own_q_ref[8:9, :]
    lane = lanes((1, 128))
    pair = turned * pltpu.roll(turned, 96, 1)
    dots = jnp.sum(query * latent, axis=1, keepdims=True)
    row = lax.broadcasted_iota(jnp.int32, (8, 128), 0)
    sums = []
    totals = []
    for s in range(2):
        here = (lane >= 64 * s) & (lane < 64 * s + 32)
        own = jnp.sum(dots[4 * s : 4 * s + 4], axis=0, keepdims=True) + jnp.sum(
            jnp.where(here, pair, 0.0), axis=1, keepdims=True
        )
        own = own * SCALE
        m = got[:, 8 + 4 * s, :] + got[:, 9 + 4 * s, :] + got[:, 10 + 4 * s, :]
        top = jnp.maximum(jnp.max(m, axis=0, keepdims=True), own)
        factor = jnp.exp(m - top)
        own_weight = jnp.exp(own - top)
        total = jnp.sum(factor * got[:, 11 + 4 * s, :], axis=0, keepdims=True)
        totals.append(total + pltpu.roll(total, 64, 1) + own_weight)
        own_low = own_weight.astype(BF16).astype(F32)
        sums.append(
            jnp.sum(got[:, 4 * s : 4 * s + 4, :] * factor[:, None, :], axis=0)
            + own_low * latent[4 * s : 4 * s + 4]
        )
    weighted_low = jnp.concatenate(sums, axis=0).astype(BF16)
    values = jnp.zeros((8, 128), F32)
    for c in range(4):
        part = jnp.dot(
            weighted_low, w_ref[128 * c : 128 * c + 128, :], preferred_element_type=F32
        )
        values = values + jnp.where(row % 4 == c, part, 0.0)
    front = jnp.sum(values[0:4], axis=0, keepdims=True) / totals[0]
    back = jnp.sum(values[4:8], axis=0, keepdims=True) / totals[1]
    attended = jnp.where(lane < 64, pltpu.roll(front, 64, 1), back).astype(BF16).astype(F32)
    out_ref[...] = jnp.broadcast_to(attended, (128, 128))


def output(tp_ref, got_ref, w_ref, other_ref, out_ref):
    first = lanes((8, 128)) < 64
    tp = tp_ref[0]
    mixed = jnp.zeros((16, 32), F32)
    for group in range(2):
        pieces = []
        for pair in range(4):
            even = got_ref[pl.ds(32 * pair + group, 8, stride=2), :]
            odd = got_ref[pl.ds(32 * pair + 16 + group, 8, stride=2), :]
            front = jnp.where(first, even, pltpu.roll(odd, 64, 1))
            back = jnp.where(first, pltpu.roll(even, 64, 1), odd)
            pieces.append(jnp.concatenate([front, back], axis=0))
        attended = jnp.concatenate(pieces, axis=1).astype(BF16)
        mine = jnp.where(tp == 0, w_ref[0:32, :], w_ref[32:64, :])
        w = jnp.where(tp == group, mine, other_ref[...])
        part = lax.dot_general(
            attended, w, (((1,), (1,)), ((), ())), preferred_element_type=F32
        )
        mixed = mixed + part.astype(BF16).astype(F32)
    out_ref[...] = mixed.astype(BF16)


def exchanged(value, axes="kv"):
    return lax.all_to_all(value, axes, split_axis=0, concat_axis=0, tiled=True)


def turn_rows(lengths, me):
    j = me % 8
    pair = jnp.stack([lengths[j], lengths[j + 8]]).astype(F32)
    inv_freq = THETA ** (-jnp.arange(ROPE // 2, dtype=F32) * 2.0 / ROPE)
    angles = pair[:, None] * inv_freq[None, :]
    cosine = jnp.cos(angles)
    sine = jnp.sin(angles)
    cosine = jnp.concatenate([cosine] * 4, axis=1).reshape(1, 128)
    sine = jnp.concatenate([-sine, sine, -sine, sine], axis=1).reshape(1, 128)
    return jnp.concatenate([cosine, sine], axis=0)


def local(
    token_state,
    norm_gain,
    wq_nope,
    wq_rope,
    w_latent,
    w_rope_key,
    kv_gain,
    w_uk,
    w_uv,
    w_out,
    latent_cache,
    rope_cache,
    lengths,
):
    me = lax.axis_index("kv").astype(jnp.int32)
    me_s = me.reshape(1)
    tp_s = lax.axis_index("tp").astype(jnp.int32).reshape(1)
    block = (64, 16, 128)
    (sent,) = call(
        project,
        [(block, BF16)],
        token_state,
        norm_gain.reshape(1, -1),
        wq_nope,
        wq_rope,
        w_latent,
        w_rope_key.T,
        w_uk,
        w_uv,
        scratch=[pltpu.VMEM(block, F32)],
    )
    sent, weights, own_q = call(
        queries,
        [(block, BF16), ((512, 128), BF16), ((16, 128), F32)],
        me_s,
        exchanged(sent),
        turn_rows(lengths, me),
        smem=(0,),
        near=(1, 2),
    )
    arrived = exchanged(sent)
    (sent,) = call(
        attend,
        [(block, BF16)],
        lengths,
        me_s,
        arrived,
        latent_cache,
        rope_cache,
        smem=(0, 1),
        near=(2,),
        far=(3, 4),
        scratch=[
            pltpu.VMEM((8, 8, 8, 128), F32),
            pltpu.VMEM((8, 8, 128), F32),
            pltpu.VMEM((8, 8, 16, 128), F32),
            pltpu.VMEM((128, 192), F32),
            pltpu.VMEM((128, 192), F32),
            pltpu.VMEM((16, 192, 512), BF16),
            pltpu.VMEM((16, 32, 192), BF16),
            pltpu.SemaphoreType.DMA((5,)),
        ],
    )
    latent_new, rope_new, own_latent, half = call(
        new_entries,
        [((16, 512), BF16), ((16, 32), BF16), ((8, 128), F32), ((32, 512), BF16)],
        me_s,
        tp_s,
        arrived,
        kv_gain.reshape(1, -1),
        w_out.T,
        smem=(0, 1),
        near=(2,),
        results_far=(0, 1),
        scratch=[pltpu.VMEM((16, 512), F32), pltpu.VMEM((8, 128), F32)],
    )
    other = lax.ppermute(half, "tp", [(0, 1), (1, 0)])
    (sent,) = call(
        combine,
        [((128, 128), F32)],
        exchanged(sent),
        weights,
        own_q,
        own_latent,
        near=(0, 1, 2, 3),
    )
    arrived = exchanged(sent.reshape(128, 1, 128), ("kv", "tp")).reshape(128, 128)
    (mixed,) = call(
        output,
        [((16, 32), BF16)],
        tp_s,
        arrived,
        w_out.T,
        other,
        smem=(0,),
        near=(1, 3),
        results_far=(0,),
    )
    return (mixed, latent_new, rope_new)


def solution(mesh):
    in_specs = (
        P("dp", "kv"),
        P("kv"),
        P("kv", "tp"),
        P("kv", "tp"),
        P("kv", None),
        P("kv", None),
        P(),
        P("kv", "tp"),
        P("kv", "tp"),
        P("tp", "kv"),
        P("dp", "kv", None),
        P("dp", None, "kv"),
        P("dp"),
    )
    out_specs = (P("dp", ("kv", "tp")), P("dp", None), P("dp", None))
    return jax.shard_map(local, mesh=mesh, in_specs=in_specs, out_specs=out_specs, check_vma=False)
```

```python
import jax
import jax.numpy as jnp
from jax import lax
from jax.experimental import pallas as pl
from jax.experimental.pallas import tpu as pltpu
from jax.sharding import PartitionSpec as P

D = 4096
NOPE = 64
ROPE = 32
V_DIM = 64
RANK = 512
EPS = 1e-06
THETA = 10000.0
NEG = -1e30
SCALE = (NOPE + ROPE) ** (-0.5)
F32 = jnp.float32
BF16 = jnp.bfloat16
INTERPRET = False


def call(kernel, outs, *args, smem=(), near=(), far=(), results_far=(), scratch=()):
    spaces = [
        pltpu.SMEM if i in smem else pl.ANY if i in far else pltpu.VMEM for i in range(len(args))
    ]
    body = kernel
    shapes = [
        jax.ShapeDtypeStruct(*out) if i in results_far else pltpu.VMEM(*out)
        for i, out in enumerate(outs)
    ]
    if len(outs) == 1 and not results_far:
        shapes.append(pltpu.VMEM((8, 128), F32))

        def body(*refs):
            refs[len(args) + 1][...] = jnp.zeros((8, 128), F32)
            kernel(*refs[: len(args) + 1], *refs[len(args) + 2 :])

    results = pl.pallas_call(
        body,
        out_shape=tuple(shapes),
        in_specs=[pl.BlockSpec(memory_space=space) for space in spaces],
        out_specs=tuple(pl.BlockSpec(memory_space=pltpu.VMEM) for _ in shapes),
        scratch_shapes=list(scratch),
        interpret=INTERPRET,
    )(
        *(
            pltpu.with_memory_space_constraint(a, pltpu.VMEM) if i in near else a
            for i, a in enumerate(args)
        )
    )
    return results[: len(outs)]


def split2(v):
    high = v.astype(BF16).astype(F32)
    return high, v - high


def split3(v):
    high, rest = split2(v)
    mid, low = split2(rest)
    return high, mid, low


def lanes(shape):
    return lax.broadcasted_iota(jnp.int32, shape, len(shape) - 1)


def turn_rows(first_length, second_length):
    lane = lanes((1, 128))
    freq = jnp.full((1, 128), 1.0, F32)
    for i in range(1, ROPE // 2):
        freq = jnp.where(lane % 16 == i, THETA ** (-2.0 * i / ROPE), freq)
    angle = jnp.where(lane < 64, first_length, second_length).astype(F32) * freq
    sine = jnp.sin(angle)
    return jnp.cos(angle), jnp.where(lane % 32 < 16, -sine, sine)


def project(
    me_ref,
    tp_ref,
    len_ref,
    x_ref,
    gain_ref,
    wn_ref,
    wr_ref,
    wl_ref,
    wk_ref,
    uk_ref,
    uv_ref,
    out_ref,
    turn_ref,
    limit_ref,
    buf,
):
    j = me_ref[0] % 8
    cosine, sine = turn_rows(len_ref[j], len_ref[j + 8])
    turn_ref[0:1, :] = cosine
    turn_ref[1:2, :] = sine
    for b in range(16):
        limit_ref[b : b + 1, :] = jnp.full((1, 256), len_ref[b], jnp.int32)
    x = x_ref[...].astype(F32)
    scaled = (x * gain_ref[...]).astype(BF16)
    nope = jnp.dot(scaled, wn_ref[...], preferred_element_type=F32)
    rope = jnp.dot(scaled, wr_ref[...], preferred_element_type=F32)
    latent = jnp.dot(scaled, wl_ref[...], preferred_element_type=F32)
    key = lax.dot_general(
        scaled, wk_ref[...], (((1,), (1,)), ((), ())), preferred_element_type=F32
    )
    squares = jnp.sum(x * x, axis=1, keepdims=True)
    first = lanes((8, 128)) < 64
    square_row = jnp.where(first, squares[:8], squares[8:])
    uk = uk_ref[...].astype(F32)
    uv = uv_ref[...].astype(F32)
    for h in range(8):
        n = slice(64 * h, 64 * h + 64)
        r = slice(32 * h, 32 * h + 32)
        c = slice(128 * (h // 2), 128 * (h // 2) + 128)
        s = slice(8 * (h % 2), 8 * (h % 2) + 8)
        weights = jnp.concatenate([uk[:, n], uv[:, n]], axis=1)
        for t in range(2):
            rows = weights[4 * t : 4 * t + 4]
            buf[t, 32 * h : 32 * h + 32, :] = jnp.concatenate([rows] * 8, axis=0)
        rows = (
            jnp.concatenate([nope[:8, n], nope[8:, n]], axis=1),
            jnp.concatenate([rope[:8, r], key[:8], rope[8:, r], key[8:]], axis=1),
            latent[s, c],
            square_row,
        )
        for i, row in enumerate(rows):
            buf[2, pl.ds(32 * h + i, 8, stride=4), :] = row
    for t in range(3):
        out_ref[:, :, 128 * t : 128 * t + 128] = buf[t].reshape(64, 4, 128).astype(BF16)


def queries(me_ref, got_ref, turn_ref, out_ref, w_ref, own_ref):
    got = got_ref[...].astype(F32)
    weights = jnp.concatenate([got[:, :, 0:128], got[:, :, 128:256]], axis=1)
    weights = weights.reshape(512, 128).astype(BF16)
    w_ref[...] = weights
    total = jnp.sum(got[:, :, 256:384], axis=0)
    nope = total[0:1]
    rope = total[1:2]
    latent = total[2:3]
    inv_rms = lax.rsqrt(total[3:4] / D + EPS)
    lane = lanes((1, 128))
    q_low = (nope * inv_rms).astype(BF16).astype(F32)
    turned = pltpu.roll(q_low, 64, 1)
    row = lax.broadcasted_iota(jnp.int32, (8, 128), 0)
    wide = lanes((8, 128))
    q_wide = jnp.where(row < 4, jnp.broadcast_to(q_low, (8, 128)), jnp.broadcast_to(turned, (8, 128)))
    q_wide = jnp.where(wide < 64, q_wide, 0.0)
    q_latent = jnp.zeros((8, 128), F32)
    for c in range(4):
        left = jnp.where(row % 4 == c, q_wide, 0.0).astype(BF16)
        q_latent = q_latent + lax.dot_general(
            left,
            weights[128 * c : 128 * c + 128],
            (((1,), (1,)), ((), ())),
            preferred_element_type=F32,
        )
    turn = rope * inv_rms
    swapped = jnp.where(lane % 32 < 16, pltpu.roll(turn, 112, 1), pltpu.roll(turn, 16, 1))
    rotated = turn * turn_ref[0:1, :] + swapped * turn_ref[1:2, :]
    other = pltpu.roll(inv_rms, 64, 1)
    odd = (me_ref[0] // 8) % 2 == 1
    latent_rms = jnp.where((lane < 64) == odd, other, inv_rms)
    high, low = split2(latent * latent_rms)
    rest = jnp.concatenate([rotated, high, low, jnp.zeros((1, 128), F32)], axis=0)
    block = jnp.concatenate([q_latent[0:4], q_latent[4:8], rest], axis=1).astype(BF16)
    own_ref[0:8, :] = q_latent.astype(BF16).astype(F32)
    own_ref[8:16, :] = jnp.broadcast_to(rotated.astype(BF16).astype(F32), (8, 128))
    out_ref[...] = jnp.broadcast_to(block[None], (64, 4, 384))


def attend(
    me_ref,
    got_ref,
    limit_ref,
    cache_hbm,
    rope_hbm,
    out_ref,
    q_buf,
    buf,
    score_buf,
    weight_buf,
    cache_ref,
    rope_ref,
    sem,
):
    copies = [pltpu.make_async_copy(rope_hbm, rope_ref, sem.at[4])] + [
        pltpu.make_async_copy(
            cache_hbm.at[4 * g : 4 * g + 4], cache_ref.at[4 * g : 4 * g + 4], sem.at[g]
        )
        for g in range(4)
    ]
    for copy in copies:
        copy.start()
    for h in range(8):
        for t in range(3):
            piece = got_ref[8 * h : 8 * h + 8, :, 128 * t : 128 * t + 128].astype(F32)
            q_buf[t, 40 * h : 40 * h + 32, :] = piece.reshape(32, 128)
    position = lanes((8, 192)) + me_ref[0] * 192
    lane = lanes((128, 128))
    copies[0].wait()
    for b in range(16):
        s, j = divmod(b, 8)
        if b % 8 == 0:
            copies[1 + b // 4].wait()
            copies[2 + b // 4].wait()
        q = [q_buf[s, pl.ds(4 * j + c, 8, stride=40), :] for c in range(4)]
        q = jnp.concatenate(q, axis=1).astype(BF16)
        q_rot = q_buf[2, pl.ds(4 * j, 8, stride=40), :][:, 64 * s : 64 * s + 32].astype(BF16)
        scores = lax.dot_general(
            q, cache_ref[b], (((1,), (1,)), ((), ())), preferred_element_type=F32
        ) + jnp.dot(q_rot, rope_ref[b], preferred_element_type=F32)
        usable = position < limit_ref[b : b + 1, 0:192]
        score_buf[8 * b : 8 * b + 8, :] = jnp.where(usable, scores * SCALE, NEG)
    masked = score_buf[...]
    top = jnp.max(masked, axis=1, keepdims=True)
    weights = jnp.where(masked > 0.5 * NEG, jnp.exp(masked - top), 0.0)
    weight_buf[...] = weights
    sum_high, sum_low = split2(jnp.sum(weights, axis=1, keepdims=True))
    high, mid, low = split3(top)
    row = jnp.where(lane < 64, jnp.where(lane < 32, high, mid), jnp.where(lane < 96, low, sum_high))
    last = jnp.broadcast_to(sum_low, (128, 128))
    for b in range(16):
        s, j = divmod(b, 8)
        buf[2, pl.ds(4 * j + 2 * s, 8, stride=40), :] = row[8 * b : 8 * b + 8]
        buf[2, pl.ds(4 * j + 2 * s + 1, 8, stride=40), :] = last[8 * b : 8 * b + 8]
    for b in range(16):
        s, j = divmod(b, 8)
        weighted = jnp.dot(
            weight_buf[8 * b : 8 * b + 8, :].astype(BF16), cache_ref[b], preferred_element_type=F32
        )
        for c in range(4):
            buf[s, pl.ds(4 * j + c, 8, stride=40), :] = weighted[:, 128 * c : 128 * c + 128]
    for h in range(8):
        for t in range(3):
            piece = buf[t, 40 * h : 40 * h + 32, :].reshape(8, 4, 128).astype(BF16)
            out_ref[8 * h : 8 * h + 8, :, 128 * t : 128 * t + 128] = piece


def new_latents(raw, gain):
    scale = lax.rsqrt(jnp.sum(raw * raw, axis=1, keepdims=True) / RANK + EPS)
    return (raw * scale * gain).astype(BF16)


def new_entries(got_ref, gain_ref, after_ref, latent_ref, rope_ref, buf):
    buf[...] = got_ref[:, :, 256:384].astype(F32).reshape(256, 128)
    turned = buf[pl.ds(0, 8, stride=4), :]
    rope_ref[...] = jnp.concatenate([turned[:, 32:64], turned[:, 96:128]], axis=0).astype(BF16)
    raw = [
        buf[pl.ds(64 * c + 1, 16, stride=4), :] + buf[pl.ds(64 * c + 2, 16, stride=4), :]
        for c in range(4)
    ]
    latent_ref[...] = new_latents(jnp.concatenate(raw, axis=1), gain_ref[...])


def combine(me_ref, got_ref, w_ref, own_q_ref, fresh_ref, gain_ref, out_ref, after_ref, buf):
    buf[...] = got_ref[:, :, 256:384].astype(F32).reshape(256, 128)
    query = own_q_ref[0:8, :]
    turned = own_q_ref[8:9, :]
    lane = lanes((1, 128))
    pair = turned * pltpu.roll(turned, 96, 1)
    j = me_ref[0] % 8
    row = lax.broadcasted_iota(jnp.int32, (8, 128), 0)
    sums = []
    totals = []
    for s in range(2):
        pieces = []
        for c in range(4):
            piece = fresh_ref[16 * c + 8 * s + j].astype(F32)[:, 256:384]
            pieces.append(piece[1:2] + piece[2:3])
        new = new_latents(jnp.concatenate(pieces, axis=1), gain_ref[...]).astype(F32)
        latent = jnp.concatenate([new[:, 128 * c : 128 * c + 128] for c in range(4)], axis=0)
        here = (lane >= 64 * s) & (lane < 64 * s + 32)
        dots = jnp.sum(query[4 * s : 4 * s + 4] * latent, axis=0, keepdims=True)
        own = jnp.sum(dots + jnp.where(here, pair, 0.0), axis=1, keepdims=True) * SCALE
        first = buf[pl.ds(2 * s, 64, stride=4), :]
        second = buf[pl.ds(2 * s + 1, 64, stride=4), :]
        m = first[:, 0:1] + first[:, 32:33] + first[:, 64:65]
        top = jnp.maximum(jnp.max(m, axis=0, keepdims=True), own)
        factor = jnp.exp(m - top)
        own_weight = jnp.exp(own - top)
        total = jnp.sum(factor * (first[:, 96:97] + second[:, 0:1]), axis=0, keepdims=True)
        totals.append(total + own_weight)
        own_low = own_weight.astype(BF16).astype(F32)
        mine = got_ref[:, :, 128 * s : 128 * s + 128].astype(F32)
        sums.append(jnp.sum(mine * factor[:, :, None], axis=0) + own_low * latent)
    weighted_low = jnp.concatenate(sums, axis=0).astype(BF16)
    values = jnp.zeros((8, 128), F32)
    for c in range(4):
        part = jnp.dot(
            weighted_low, w_ref[128 * c : 128 * c + 128, :], preferred_element_type=F32
        )
        values = values + jnp.where(row % 4 == c, part, 0.0)
    front = jnp.sum(values[0:4], axis=0, keepdims=True) / totals[0]
    back = jnp.sum(values[4:8], axis=0, keepdims=True) / totals[1]
    attended = jnp.where(lane < 64, pltpu.roll(front, 64, 1), back).astype(BF16).astype(F32)
    out_ref[...] = jnp.broadcast_to(attended, (128, 128))
    after_ref[...] = jnp.zeros((8, 128), F32)


def half_of(tp_ref, w_ref, after_ref, half_ref):
    half_ref[...] = jnp.where(tp_ref[0] == 0, w_ref[32:64, :], w_ref[0:32, :])


def output(tp_ref, got_ref, w_ref, other_ref, out_ref):
    first = lanes((8, 128)) < 64
    tp = tp_ref[0]
    mixed = jnp.zeros((16, 32), F32)
    for group in range(2):
        pieces = []
        for pair in range(4):
            even = got_ref[pl.ds(32 * pair + group, 8, stride=2), :]
            odd = got_ref[pl.ds(32 * pair + 16 + group, 8, stride=2), :]
            front = jnp.where(first, even, pltpu.roll(odd, 64, 1))
            back = jnp.where(first, pltpu.roll(even, 64, 1), odd)
            pieces.append(jnp.concatenate([front, back], axis=0))
        attended = jnp.concatenate(pieces, axis=1).astype(BF16)
        mine = jnp.where(tp == 0, w_ref[0:32, :], w_ref[32:64, :])
        w = jnp.where(tp == group, mine, other_ref[...])
        part = lax.dot_general(
            attended, w, (((1,), (1,)), ((), ())), preferred_element_type=F32
        )
        mixed = mixed + part.astype(BF16).astype(F32)
    out_ref[...] = mixed.astype(BF16)


def exchanged(value, axes="kv"):
    return lax.all_to_all(value, axes, split_axis=0, concat_axis=0, tiled=True)


def local(
    token_state,
    norm_gain,
    wq_nope,
    wq_rope,
    w_latent,
    w_rope_key,
    kv_gain,
    w_uk,
    w_uv,
    w_out,
    latent_cache,
    rope_cache,
    lengths,
):
    me = lax.axis_index("kv").astype(jnp.int32).reshape(1)
    tp = lax.axis_index("tp").astype(jnp.int32).reshape(1)
    gain = kv_gain.reshape(1, -1)
    w_turned = w_out.T
    block = (64, 4, 384)
    sent, turn, limits = call(
        project,
        [(block, BF16), ((8, 128), F32), ((16, 256), jnp.int32)],
        me,
        tp,
        lengths,
        token_state,
        norm_gain.reshape(1, -1),
        wq_nope,
        wq_rope,
        w_latent,
        w_rope_key.T,
        w_uk,
        w_uv,
        smem=(0, 1, 2),
        scratch=[pltpu.VMEM((3, 256, 128), F32)],
    )
    sent, weights, own_q = call(
        queries,
        [(block, BF16), ((512, 128), BF16), ((16, 128), F32)],
        me,
        exchanged(sent),
        turn,
        smem=(0,),
        near=(1, 2),
    )
    fresh = exchanged(sent)
    (sent,) = call(
        attend,
        [(block, BF16)],
        me,
        fresh,
        limits,
        latent_cache,
        rope_cache,
        smem=(0,),
        near=(1, 2),
        far=(3, 4),
        scratch=[
            pltpu.VMEM((3, 320, 128), F32),
            pltpu.VMEM((3, 320, 128), F32),
            pltpu.VMEM((128, 192), F32),
            pltpu.VMEM((128, 192), F32),
            pltpu.VMEM((16, 192, 512), BF16),
            pltpu.VMEM((16, 32, 192), BF16),
            pltpu.SemaphoreType.DMA((5,)),
        ],
    )
    sent, after = call(
        combine,
        [((128, 128), F32), ((8, 128), F32)],
        me,
        exchanged(sent),
        weights,
        own_q,
        fresh,
        gain,
        smem=(0,),
        near=(1, 2, 3, 4, 5),
        scratch=[pltpu.VMEM((256, 128), F32)],
    )
    arrived = exchanged(sent.reshape(128, 1, 128), ("kv", "tp")).reshape(128, 128)
    (half,) = call(
        half_of,
        [((32, 512), BF16)],
        tp,
        w_turned,
        after,
        smem=(0,),
        near=(1, 2),
    )
    other = lax.ppermute(half, "tp", [(0, 1), (1, 0)])
    latent_new, rope_new = call(
        new_entries,
        [((16, 512), BF16), ((16, 32), BF16)],
        fresh,
        gain,
        after,
        near=(0, 1, 2),
        results_far=(0, 1),
        scratch=[pltpu.VMEM((256, 128), F32)],
    )
    (mixed,) = call(
        output,
        [((16, 32), BF16)],
        tp,
        arrived,
        w_turned,
        other,
        smem=(0,),
        near=(1, 2, 3),
        results_far=(0,),
    )
    return (mixed, latent_new, rope_new)


def solution(mesh):
    in_specs = (
        P("dp", "kv"),
        P("kv"),
        P("kv", "tp"),
        P("kv", "tp"),
        P("kv", None),
        P("kv", None),
        P(),
        P("kv", "tp"),
        P("kv", "tp"),
        P("tp", "kv"),
        P("dp", "kv", None),
        P("dp", None, "kv"),
        P("dp"),
    )
    out_specs = (P("dp", ("kv", "tp")), P("dp", None), P("dp", None))
    return jax.shard_map(local, mesh=mesh, in_specs=in_specs, out_specs=out_specs, check_vma=False)
```
